32 devices in a mesh: sp: 8 (over z, x), tp: 4 (over y, core).
Axes of the slice: x: 2, y: 2, z: 4, core: 2. Of those that a mesh axis runs over, the one named last changes fastest.
Arguments:
- out_grad: bfloat16 [1024, 2048], P('sp', 'tp'), may hold values from -6 to 6
- moe_input: bfloat16 [1024, 2048], P('sp', 'tp'), may hold values from -6 to 6
- route_weight: float32 [1024, 2], P('sp'), may hold values from 0.2 to 1
- route_ids: int32 [1024, 2], P('sp'), may hold values from 0 to 7, all different within a row; in each aligned block of 128 rows (0 to 127, 128 to 255, ...) at most 64 rows name the same one
- gate_proj: bfloat16 [8, 2048, 2816], P('sp', None, 'tp'), may hold values from -0.125 to 0.125
- up_proj: bfloat16 [8, 2048, 2816], P('sp', None, 'tp'), may hold values from -0.125 to 0.125
- down_proj: bfloat16 [8, 2816, 2048], P('sp', 'tp'), may hold values from -0.109375 to 0.109375
- out_proj: bfloat16 [2048, 2048], P(None, 'tp'), may hold values from -0.125 to 0.125
- conv_out: bfloat16 [1024, 2048], P('sp', 'tp'), may hold values from -6 to 6
- gate_b: bfloat16 [1024, 2048], P('sp', 'tp'), may hold values from -6 to 6
- gate_c: bfloat16 [1024, 2048], P('sp', 'tp'), may hold values from -6 to 6
- value_v: bfloat16 [1024, 2048], P('sp', 'tp'), may hold values from -6 to 6
- conv_taps: float32 [3, 2048], P(None, 'tp'), may hold values from -3 to 3
Outputs:
- grad_gate: bfloat16 [8, 2048, 2816], P('sp', None, 'tp')
- grad_up: bfloat16 [8, 2048, 2816], P('sp', None, 'tp')
- grad_down: bfloat16 [8, 2816, 2048], P('sp', 'tp')
- grad_out: float32 [2048, 2048], P('sp', 'tp')
- grad_b: bfloat16 [1024, 2048], P('sp', 'tp')
- grad_c: bfloat16 [1024, 2048], P('sp', 'tp')
- grad_v: bfloat16 [1024, 2048], P('sp', 'tp')
The draws below stay inside these ranges and needn't reach their ends.
Inputs may be any that keep to these rules, and one draw needn't show every extreme that they name: `route_ids`: each row names two different experts; within the 128 rows of one index of sp no expert is named by more than 64 rows, a bound that some block reaches.
All inputs are finite; a program needn't handle non-finite values.
Results may differ from the reference program's by a relative error of at most 0.019.
Values may be sent and summed in bfloat16 or wider, within the bound.
A program may use at most 64 MiB of HBM per device.

```python
import math
import jax
import jax.numpy as jnp
import numpy as np
from jax import lax

D = 2048
FF = 2816
TOK_DEV = 128
TOKENS = 1024
EXPERTS = 8
CAP = 64
N_SP = 8
N_TP = 4


def with_spikes(drawn, key, source, target, shards_of, factor):
    owner, partner = [(jnp.arange(drawn.shape[axis_at]) // (drawn.shape[axis_at] // shards_of)).reshape([-1 if axis == axis_at else 1 for axis in range(drawn.ndim)]) for axis_at in (source, target)]
    chosen = jax.random.permutation(key, shards_of)[partner]
    strong = (owner == chosen) | (owner == (partner + shards_of // 2) % shards_of)
    return jnp.where(strong, factor * drawn, drawn)


def block_levels(rng, shape, pieces, smallest, top_value):
    def one(axis_at, blocks):
        heights = jax.random.uniform(jax.random.fold_in(jax.random.fold_in(rng, 6), axis_at), (blocks,), jnp.float32, smallest / len(pieces), top_value / len(pieces))
        return jnp.repeat(jnp.exp(heights), shape[axis_at] // blocks).reshape((-1,) + (1,) * (len(shape) - axis_at - 1))

    level = one(*pieces[0])
    for cut in pieces[1:]:
        level = level * one(*cut)
    return level


def routed_block(key, own, number, rows, amount, top, bound, skew):
    order = jax.random.permutation(key, amount)
    crowded, ordinary = portions_of(amount, rows * top, bound, skew, True), portions_of(amount, rows * top, bound, skew, False)
    places = jnp.arange(amount)

    def named(sizes, rotation):
        used = int((sizes > 0).sum())
        fixed = max(1, used // 4)
        passed = fixed + (places - fixed + rotation * (used - fixed)) % max(1, amount - fixed)
        return jnp.zeros((amount,), jnp.int32).at[order[jnp.where(places < fixed, places, passed)]].set(jnp.asarray(sizes, jnp.int32))

    sizes = jnp.where(number % 4 == 0, named(crowded, number // 4), named(ordinary, number - number // 4 - 1))
    mixed = jax.random.permutation(jax.random.fold_in(own, 3), amount)
    donor, sink = mixed[0:amount // 2 * 2:2], mixed[1:amount // 2 * 2:2]
    room = jnp.minimum(sizes[donor] - 1, bound - sizes[sink]) // 2
    room = jnp.where((donor == order[0]) | (sink == order[0]) | (sizes[sink] == 0), 0, jnp.maximum(room, 0))
    passed = jax.random.randint(jax.random.fold_in(own, 4), (amount // 2,), 0, 1 << 20) % (room + 1)
    sizes = sizes.at[donor].add(-passed).at[sink].add(passed)
    labels = jnp.searchsorted(jnp.cumsum(sizes), jnp.arange(rows * top), side="right").astype(jnp.int32)
    grid = labels.reshape(top, rows).T
    grid = grid[jax.random.permutation(jax.random.fold_in(own, 1), rows)]
    rotation = jax.random.randint(jax.random.fold_in(own, 2), (rows, 1), 0, top)
    return jnp.take_along_axis(grid, (jnp.arange(top)[None, :] + rotation) % top, axis=1)


def portions_of(count, total, most, skew, full):
    weights = [(1 << 20) // math.isqrt(standing ** skew) + 1 for standing in range(1, count + 1)]
    largest = most if full else min(most, max(-(-total // count), total * weights[0] // sum(weights)))
    least = 1 if total - largest >= count - 1 else 0
    given, surplus = [largest] + [least] * (count - 1), total - largest - least * (count - 1)
    while surplus > 0:
        movable = [i for i in range(1, count) if given[i] < largest] or [i for i in range(1, count) if given[i] < most]
        mass, left = sum([weights[i] for i in movable]), surplus
        for i in movable:
            addition = min(most - given[i], max(1, left * weights[i] // mass), surplus)
            given[i] = given[i] + addition
            surplus = surplus - addition
    return np.array(given)


def normal_values(rng, shape, deviation, reach, split=(), kind=jnp.bfloat16):
    loudness = block_levels(rng, shape, split, -0.22, 0.18) if split else 1.0
    values = jax.random.normal(rng, shape, jnp.float32) * deviation * loudness
    return jnp.minimum(jnp.maximum(values, -reach), reach).astype(kind)


def bell_draw_with(rng, extent, spread, limit, pieces, heavy, held_as=jnp.bfloat16):
    array = spread * jax.random.normal(rng, extent, jnp.float32)
    if pieces:
        array = array * block_levels(rng, extent, pieces, -0.22, 0.18)
    return jnp.clip(with_spikes(array, jax.random.fold_in(rng, 3), *heavy), -limit, limit).astype(held_as)


def setup_inputs(seed: int = 0) -> dict:
    arg_keys = jax.random.split(jax.random.key(seed), 14)
    out_grad = bell_draw_with(arg_keys[0], (TOKENS, D), 1.0, 6.0, ((0, 8), (1, 4)), (0, 1, 8, 2.0))
    moe_input = normal_values(arg_keys[1], (TOKENS, D), 1.0, 6.0, ((0, 8), (1, 4)))
    route_weight = jnp.clip(jnp.exp(math.log(1.0) - 1.609438 * jax.random.uniform(arg_keys[2], (TOKENS, 2), jnp.float32) ** block_levels(arg_keys[2], (TOKENS, 2), ((0, 8),), -0.2, 0.2)), 0.2, 1.0)
    route_ids_keys = jax.random.split(jax.random.fold_in(arg_keys[3], 1), TOKENS // TOK_DEV)
    route_ids_turns = jax.random.permutation(jax.random.fold_in(arg_keys[3], 3), TOKENS // TOK_DEV)
    route_ids = jax.vmap(lambda own, number: routed_block(jax.random.fold_in(arg_keys[3], 2), own, number, TOK_DEV, EXPERTS, 2, CAP, 1))(route_ids_keys, route_ids_turns).reshape((TOKENS, 2))
    gate_proj = normal_values(arg_keys[4], (EXPERTS, D, FF), D ** -0.5, 0.125, ((0, 8), (2, 4)))
    up_proj = normal_values(arg_keys[5], (EXPERTS, D, FF), D ** -0.5, 0.125, ((0, 8), (2, 4)))
    down_proj = normal_values(arg_keys[6], (EXPERTS, FF, D), FF ** -0.5, 0.109375, ((0, 8), (1, 4)))
    out_proj = normal_values(arg_keys[7], (D, D), D ** -0.5, 0.125, ((1, 4),))
    conv_out = normal_values(arg_keys[8], (TOKENS, D), 1.0, 6.0, ((0, 8), (1, 4)))
    gate_b = normal_values(arg_keys[9], (TOKENS, D), 1.0, 6.0, ((0, 8), (1, 4)))
    gate_c = normal_values(arg_keys[10], (TOKENS, D), 1.0, 6.0, ((0, 8), (1, 4)))
    value_v = normal_values(arg_keys[11], (TOKENS, D), 1.0, 6.0, ((0, 8), (1, 4)))
    conv_taps = normal_values(arg_keys[12], (3, D), 0.6, 3.0, ((1, 4),), jnp.float32)
    return {"out_grad": out_grad, "moe_input": moe_input, "route_weight": route_weight, "route_ids": route_ids, "gate_proj": gate_proj, "up_proj": up_proj, "down_proj": down_proj, "out_proj": out_proj, "conv_out": conv_out, "gate_b": gate_b, "gate_c": gate_c, "value_v": value_v, "conv_taps": conv_taps}


def slot_table(route_ids):
    flat = route_ids.reshape(N_SP, TOK_DEV * 2).astype(jnp.int32)
    onehot = (flat[:, :, None] == jnp.arange(EXPERTS, dtype=jnp.int32)[None, None, :]).astype(jnp.int32)
    before = jnp.cumsum(onehot, axis=1) - onehot
    slot = jnp.sum(before * onehot, axis=2).astype(jnp.int32)
    return (flat * CAP + slot).astype(jnp.int32)


def place_rows(rows, index):
    return jnp.zeros((EXPERTS * CAP, rows.shape[1]), rows.dtype).at[index].set(rows)


def reference(out_grad, moe_input, route_weight, route_ids, gate_proj, up_proj, down_proj, out_proj, conv_out, gate_b, gate_c, value_v, conv_taps):
    dest = slot_table(route_ids)
    sent = (route_weight[:, :, None] * out_grad.astype(jnp.float32)[:, None, :]).astype(jnp.bfloat16)
    rows_x = jnp.broadcast_to(moe_input[:, None, :], (TOKENS, 2, D)).reshape(N_SP, 2 * TOK_DEV, D)
    rows_dy = sent.reshape(N_SP, 2 * TOK_DEV, D)
    slots_x = jax.vmap(place_rows)(rows_x, dest).reshape(N_SP, EXPERTS, CAP, D)
    slots_dy = jax.vmap(place_rows)(rows_dy, dest).reshape(N_SP, EXPERTS, CAP, D)
    width = FF // N_TP

    def expert(index):
        xin = slots_x[:, index].reshape(N_SP * CAP, D)
        dyin = slots_dy[:, index].reshape(N_SP * CAP, D)
        w_gate = gate_proj[index]
        w_up = up_proj[index]
        w_down = down_proj[index]
        gate = jnp.dot(xin, w_gate, preferred_element_type=jnp.float32)
        upval = jnp.dot(xin, w_up, preferred_element_type=jnp.float32)
        sig = jax.nn.sigmoid(gate)
        act = gate * sig
        hidden = (act * upval).astype(jnp.bfloat16)
        g_down = jnp.dot(hidden.T, dyin, preferred_element_type=jnp.float32).astype(jnp.bfloat16)
        dhid = jnp.dot(dyin, w_down.T, preferred_element_type=jnp.float32)
        dgate = (dhid * upval * (sig * (1.0 + gate * (1.0 - sig)))).astype(jnp.bfloat16)
        dup = (dhid * act).astype(jnp.bfloat16)
        g_gate = jnp.dot(xin.T, dgate, preferred_element_type=jnp.float32).astype(jnp.bfloat16)
        g_up = jnp.dot(xin.T, dup, preferred_element_type=jnp.float32).astype(jnp.bfloat16)
        rows = N_SP * CAP
        part = jnp.einsum('rpf,dpf->prd', dgate.reshape(rows, N_TP, width).astype(jnp.float32),
                          w_gate.reshape(D, N_TP, width).astype(jnp.float32))
        part = part + jnp.einsum('rpf,dpf->prd', dup.reshape(rows, N_TP, width).astype(jnp.float32),
                                 w_up.reshape(D, N_TP, width).astype(jnp.float32))
        part = lax.optimization_barrier(part.astype(jnp.bfloat16)).astype(jnp.float32)
        back = jnp.sum(part, axis=0).astype(jnp.bfloat16)
        return g_gate, g_up, g_down, back

    grad_gate, grad_up, grad_down, backs = lax.map(expert, jnp.arange(EXPERTS, dtype=jnp.int32))
    backs = backs.reshape(EXPERTS, N_SP, CAP, D).transpose(1, 0, 2, 3).reshape(N_SP, EXPERTS * CAP, D)
    picked = jax.vmap(lambda table, index: table[index])(backs, dest)
    moe_grad = jnp.sum(picked.reshape(TOKENS, 2, D).astype(jnp.float32), axis=1)
    grad_h = (out_grad.astype(jnp.float32) + moe_grad).astype(jnp.bfloat16)
    grad_z = jnp.dot(grad_h, out_proj, preferred_element_type=jnp.float32)
    dconv = (grad_z * gate_b.astype(jnp.float32)).astype(jnp.bfloat16)
    grad_b = (grad_z * conv_out.astype(jnp.float32)).astype(jnp.bfloat16)
    padded = jnp.pad(dconv.astype(jnp.float32), ((1, 1), (0, 0)))
    grad_u = conv_taps[0] * padded[2:] + conv_taps[1] * padded[1:-1] + conv_taps[2] * padded[:-2]
    grad_c = (grad_u * value_v.astype(jnp.float32)).astype(jnp.bfloat16)
    grad_v = (grad_u * gate_c.astype(jnp.float32)).astype(jnp.bfloat16)
    mixed = (gate_b.astype(jnp.float32) * conv_out.astype(jnp.float32)).astype(jnp.bfloat16)
    grad_out = jnp.dot(grad_h.T, mixed, preferred_element_type=jnp.float32)
    return grad_gate, grad_up, grad_down, grad_out, grad_b, grad_c, grad_v
```

```python
import functools

import jax
import jax.numpy as jnp
from jax import lax
from jax.experimental import pallas as pl
from jax.experimental.pallas import tpu as pltpu
from jax.sharding import PartitionSpec as P

MESH = pl.DeviceIdType.MESH


def place(n, q):
    s, t = lax.axis_index("sp"), lax.axis_index("tp")
    sibling = t + 1 - 2 * lax.rem(t, 2)
    return s, t, sibling


def greet(n, q):
    s, t, sibling = place(n, q)
    barrier = pltpu.get_barrier_semaphore()
    for i in range(1, n):
        pl.semaphore_signal(
            barrier, inc=1, device_id=(lax.rem(s + i, n), t), device_id_type=MESH
        )
    for d in range(1, q // 2):
        pl.semaphore_signal(
            barrier, inc=1, device_id=(s, lax.rem(t + 2 * d, q)), device_id_type=MESH
        )
    pl.semaphore_signal(barrier, inc=1, device_id=(s, sibling), device_id_type=MESH)
    return barrier, n - 1 + q // 2


def remote(src, dst, send_sem, recv_sem, device):
    return pltpu.make_async_remote_copy(
        src_ref=src,
        dst_ref=dst,
        send_sem=send_sem,
        recv_sem=recv_sem,
        device_id=device,
        device_id_type=MESH,
    )


def dispatch_kernel(
    n, q, ids_ref, w_ref, x_ref, g_ref, xo_ref, do_ref, p_ref,
    p01, send, buf, out_sem, s1, r1, sy, ry, ss, rs,
):
    s, t, sibling = place(n, q)
    ny = q // 2
    tok, cols = x_ref.shape
    total = send.shape[1]
    cap = total // n
    barrier, greeted = greet(n, q)

    ids0, ids1 = ids_ref[0:1, :], ids_ref[1:2, :]
    experts = lax.broadcasted_iota(jnp.int32, (n, tok), 0)
    named = jnp.logical_or(ids0 == experts, ids1 == experts)
    named_f = jnp.where(named, 1.0, 0.0)
    earlier = jnp.where(
        lax.broadcasted_iota(jnp.int32, (tok, tok), 0)
        < lax.broadcasted_iota(jnp.int32, (tok, tok), 1),
        1.0,
        0.0,
    )
    before = jnp.dot(
        named_f.astype(jnp.bfloat16),
        earlier.astype(jnp.bfloat16),
        preferred_element_type=jnp.float32,
    ).astype(jnp.int32)
    slots = lax.broadcasted_iota(jnp.int32, (cap, tok), 0)
    for e in range(n):
        here = before[e : e + 1, :] == slots
        c0 = jnp.where(jnp.logical_and(here, ids0 == e), 1.0, 0.0)
        c1 = jnp.where(jnp.logical_and(here, ids1 == e), 1.0, 0.0)
        rows = slice(e * cap, (e + 1) * cap)
        p01[rows, 0:tok] = c0.astype(jnp.bfloat16)
        p01[rows, tok : 2 * tok] = c1.astype(jnp.bfloat16)
        p_ref[rows, :] = (c0 + c1).astype(jnp.bfloat16)
    grad = g_ref[...].astype(jnp.float32)
    weighted = jnp.concatenate(
        [
            (w_ref[:, 0:1] * grad).astype(jnp.bfloat16),
            (w_ref[:, 1:2] * grad).astype(jnp.bfloat16),
        ],
        axis=0,
    )
    send[0] = jnp.dot(p_ref[...], x_ref[...], preferred_element_type=jnp.float32).astype(
        jnp.bfloat16
    )
    send[1] = jnp.dot(p01[...], weighted, preferred_element_type=jnp.float32).astype(jnp.bfloat16)

    def at_rows(j):
        return pl.ds(pl.multiple_of(j * cap, cap), cap)

    def block(j, tt):
        return buf.at[:, at_rows(j), pl.ds(pl.multiple_of(tt * cols, cols), cols)]

    def first(i):
        e = lax.rem(s + i, n)
        return remote(send.at[:, at_rows(e)], block(s, t), s1.at[i], r1.at[i], (e, t))

    def across(i, d):
        j = lax.rem(s - i + n, n)
        b = block(j, t)
        return remote(b, b, sy.at[i, d - 1], ry.at[i, d - 1], (s, lax.rem(t + 2 * d, q)))

    def beside(i, d):
        j = lax.rem(s - i + n, n)
        b = block(j, lax.rem(t - 2 * d + q, q))
        return remote(b, b, ss.at[i, d], rs.at[i, d], (s, sibling))

    pl.semaphore_wait(barrier, greeted)
    own = pltpu.make_async_copy(send.at[:, at_rows(s)], block(s, t), s1.at[0])
    own.start()
    for i in range(1, n):
        first(i).start()

    def forward(i):
        for d in range(1, ny):
            across(i, d).wait_recv()
            beside(i, d).start()

    outs = []

    def drain(i):
        j = lax.rem(s - i + n, n)
        for d in range(ny):
            beside(i, d).wait_recv()
        for a, ref in enumerate((xo_ref, do_ref)):
            copy = pltpu.make_async_copy(
                buf.at[a, at_rows(j)], ref.at[at_rows(j)], out_sem.at[i, a]
            )
            copy.start()
            outs.append(copy)

    for i in range(n):
        if i == 0:
            own.wait()
        else:
            first(i).wait_recv()
        for d in range(1, ny):
            across(i, d).start()
        beside(i, 0).start()
        if i >= 1:
            forward(i - 1)
        if i >= 2:
            drain(i - 2)
    forward(n - 1)
    for i in range(max(n - 2, 0), n):
        drain(i)
    for i in range(n):
        if i:
            first(i).wait_send()
        for d in range(1, ny):
            across(i, d).wait_send()
        for d in range(ny):
            beside(i, d).wait_send()
    for copy in outs:
        copy.wait()


def dispatch(n, q, ids_t, weight, x, g):
    tok, cols = x.shape
    total = 4 * tok
    ny = q // 2
    vmem = pl.BlockSpec(memory_space=pltpu.VMEM)
    hbm = pl.BlockSpec(memory_space=pl.ANY)
    dma = pltpu.SemaphoreType.DMA
    rows = jax.ShapeDtypeStruct((total, q * cols), jnp.bfloat16)
    return pl.pallas_call(
        functools.partial(dispatch_kernel, n, q),
        out_shape=(rows, rows, jax.ShapeDtypeStruct((total, tok), jnp.bfloat16)),
        in_specs=[vmem] * 4,
        out_specs=(hbm, hbm, vmem),
        scratch_shapes=[
            pltpu.VMEM((total, 2 * tok), jnp.bfloat16),
            pltpu.VMEM((2, total, cols), jnp.bfloat16),
            pltpu.VMEM((2, total, q * cols), jnp.bfloat16),
            dma((n, 2)),
            dma((n,)),
            dma((n,)),
            dma((n, max(ny - 1, 1))),
            dma((n, max(ny - 1, 1))),
            dma((n, ny)),
            dma((n, ny)),
        ],
        compiler_params=pltpu.CompilerParams(collective_id=0, has_side_effects=True),
        name="dispatch",
    )(ids_t, weight, x, g)


def combine_kernel(
    n, q, part_ref, p_ref, g_ref, h_ref,
    rsib, pair, ryb, fin, ret, ss, rs, sy, ry, s3, r3,
):
    s, t, sibling = place(n, q)
    ny = q // 2
    tok, cols = g_ref.shape
    total = part_ref.shape[0]
    cap = total // n
    barrier, greeted = greet(n, q)

    def at_rows(j):
        return pl.ds(pl.multiple_of(j * cap, cap), cap)

    def at_cols(tt):
        return pl.ds(pl.multiple_of(tt * cols, cols), cols)

    def beside(i, d):
        j = lax.rem(s + i, n)
        theirs = lax.rem(sibling + 2 * d, q)
        return remote(
            part_ref.at[at_rows(j), at_cols(theirs)],
            rsib.at[d, at_rows(j)],
            ss.at[i, d],
            rs.at[i, d],
            (s, sibling),
        )

    def across(i, d):
        j = lax.rem(s + i, n)
        return remote(
            pair.at[d - 1, at_rows(j)],
            ryb.at[d - 1, at_rows(j)],
            sy.at[i, d - 1],
            ry.at[i, d - 1],
            (s, lax.rem(t + 2 * d, q)),
        )

    def back(i):
        j = lax.rem(s + i, n)
        return remote(fin.at[at_rows(j)], ret.at[at_rows(s)], s3.at[i], r3.at[i], (j, t))

    def mine(j, d):
        value = part_ref[at_rows(j), at_cols(lax.rem(t + 2 * d, q))].astype(jnp.float32)
        return value + rsib[d, at_rows(j), :].astype(jnp.float32)

    order = [i % n for i in range(1, n + 1)]
    pl.semaphore_wait(barrier, greeted)
    for i in order:
        for d in [*range(1, ny), 0]:
            beside(i, d).start()

    def finish(i):
        j = lax.rem(s + i, n)
        beside(i, 0).wait_recv()
        value = mine(j, 0)
        for d in range(1, ny):
            across(i, d).wait_recv()
            value = value + ryb[d - 1, at_rows(j), :].astype(jnp.float32)
        value = value.astype(jnp.bfloat16)
        if i == 0:
            ret[at_rows(s), :] = value
        else:
            fin[at_rows(j), :] = value
            back(i).start()

    for k, i in enumerate(order):
        j = lax.rem(s + i, n)
        for d in range(1, ny):
            beside(i, d).wait_recv()
            pair[d - 1, at_rows(j), :] = mine(j, d).astype(jnp.bfloat16)
            across(i, d).start()
        if k >= 1:
            finish(order[k - 1])
    finish(order[-1])
    for i in range(1, n):
        back(i).wait_recv()
    moe = lax.dot_general(
        p_ref[...], ret[...], (((0,), (0,)), ((), ())), preferred_element_type=jnp.float32
    )
    h_ref[...] = (g_ref[...].astype(jnp.float32) + moe).astype(jnp.bfloat16)
    for i in range(n):
        if i:
            back(i).wait_send()
        for d in range(1, ny):
            across(i, d).wait_send()
        for d in range(ny):
            beside(i, d).wait_send()


def combine(n, q, part, p, g):
    total = part.shape[0]
    cols = g.shape[1]
    ny = q // 2
    far = max(ny - 1, 1)
    vmem = pl.BlockSpec(memory_space=pltpu.VMEM)
    dma = pltpu.SemaphoreType.DMA
    return pl.pallas_call(
        functools.partial(combine_kernel, n, q),
        out_shape=jax.ShapeDtypeStruct(g.shape, jnp.bfloat16),
        in_specs=[vmem] * 3,
        out_specs=vmem,
        scratch_shapes=[
            pltpu.VMEM((ny, total, cols), jnp.bfloat16),
            pltpu.VMEM((far, total, cols), jnp.bfloat16),
            pltpu.VMEM((far, total, cols), jnp.bfloat16),
            pltpu.VMEM((total, cols), jnp.bfloat16),
            pltpu.VMEM((total, cols), jnp.bfloat16),
            dma((n, ny)),
            dma((n, ny)),
            dma((n, far)),
            dma((n, far)),
            dma((n,)),
            dma((n,)),
        ],
        compiler_params=pltpu.CompilerParams(collective_id=1, has_side_effects=True),
        name="combine",
    )(part, p, g)


def with_halo(block, sides, width):
    for axis, dim in sides:
        count = lax.axis_size(axis)
        forward = [(i, i + 1) for i in range(count - 1)]
        backward = [(target, source) for source, target in forward]
        low = lax.ppermute(
            lax.slice_in_dim(block, block.shape[dim] - width, None, axis=dim), axis, forward
        )
        high = lax.ppermute(lax.slice_in_dim(block, 0, width, axis=dim), axis, backward)
        block = jnp.concatenate([low, block, high], axis=dim)
    return block


def local(
    out_grad,
    moe_input,
    route_weight,
    route_ids,
    gate_proj,
    up_proj,
    down_proj,
    out_proj,
    conv_out,
    gate_b,
    gate_c,
    value_v,
    conv_taps,
):
    n = lax.axis_size("sp")
    q = lax.axis_size("tp")
    tok_rows = out_grad.shape[0]
    mixed = (gate_b.astype(jnp.float32) * conv_out.astype(jnp.float32)).astype(jnp.bfloat16)
    xin, dyin, slots = dispatch(n, q, route_ids.T, route_weight, moe_input, out_grad)
    w_gate = gate_proj[0]
    w_up = up_proj[0]
    w_down = down_proj[0]
    gate = jnp.dot(xin, w_gate, preferred_element_type=jnp.float32)
    upval = jnp.dot(xin, w_up, preferred_element_type=jnp.float32)
    sig = jax.nn.sigmoid(gate)
    act = gate * sig
    hidden = (act * upval).astype(jnp.bfloat16)
    dhid = jnp.dot(dyin, w_down.T, preferred_element_type=jnp.float32)
    dgate = (dhid * upval * (sig * (1.0 + gate * (1.0 - sig)))).astype(jnp.bfloat16)
    dup = (dhid * act).astype(jnp.bfloat16)
    partial_value = jnp.dot(dgate, w_gate.T, preferred_element_type=jnp.float32) + jnp.dot(
        dup, w_up.T, preferred_element_type=jnp.float32
    )
    grad_h = combine(n, q, partial_value.astype(jnp.bfloat16), slots, out_grad)
    grad_down = jnp.dot(hidden.T, dyin, preferred_element_type=jnp.float32).astype(jnp.bfloat16)
    grad_gate = jnp.dot(xin.T, dgate, preferred_element_type=jnp.float32).astype(jnp.bfloat16)
    grad_up = jnp.dot(xin.T, dup, preferred_element_type=jnp.float32).astype(jnp.bfloat16)
    full_h = lax.all_gather(grad_h, "tp", axis=1, tiled=True)
    width = full_h.shape[1]
    all_mixed = lax.all_gather(mixed, "sp", axis=0, tiled=True)
    sent_h = full_h.reshape(tok_rows, n, width // n).transpose(1, 0, 2)
    all_h = lax.all_to_all(sent_h, "sp", split_axis=0, concat_axis=0, tiled=True)
    grad_z = jnp.dot(full_h, out_proj, preferred_element_type=jnp.float32)
    dconv = (grad_z * gate_b.astype(jnp.float32)).astype(jnp.bfloat16)
    grad_b = (grad_z * conv_out.astype(jnp.float32)).astype(jnp.bfloat16)
    padded = with_halo(dconv, (("sp", 0),), 1).astype(jnp.float32)
    grad_u = conv_taps[0] * padded[2:] + conv_taps[1] * padded[1:-1] + conv_taps[2] * padded[:-2]
    grad_c = (grad_u * value_v.astype(jnp.float32)).astype(jnp.bfloat16)
    grad_v = (grad_u * gate_c.astype(jnp.float32)).astype(jnp.bfloat16)
    grad_out = lax.dot_general(
        all_h.reshape(n * tok_rows, width // n),
        all_mixed,
        (((0,), (0,)), ((), ())),
        preferred_element_type=jnp.float32,
    )
    return (grad_gate[None], grad_up[None], grad_down[None], grad_out, grad_b, grad_c, grad_v)


def solution(mesh):
    in_specs = (
        P("sp", "tp"),
        P("sp", "tp"),
        P("sp", None),
        P("sp", None),
        P("sp", None, "tp"),
        P("sp", None, "tp"),
        P("sp", "tp", None),
        P(None, "tp"),
        P("sp", "tp"),
        P("sp", "tp"),
        P("sp", "tp"),
        P("sp", "tp"),
        P(None, "tp"),
    )
    out_specs = (
        P("sp", None, "tp"),
        P("sp", None, "tp"),
        P("sp", "tp", None),
        P("sp", "tp"),
        P("sp", "tp"),
        P("sp", "tp"),
        P("sp", "tp"),
    )
    return jax.shard_map(local, mesh=mesh, in_specs=in_specs, out_specs=out_specs, check_vma=False)
```

```python
import functools

import jax
import jax.numpy as jnp
from jax import lax
from jax.experimental import pallas as pl
from jax.experimental.pallas import tpu as pltpu
from jax.sharding import PartitionSpec as P

MESH = pl.DeviceIdType.MESH


def place(n, q):
    s, t = lax.axis_index("sp"), lax.axis_index("tp")
    sibling = t + 1 - 2 * lax.rem(t, 2)
    return s, t, sibling


def greet(n, q):
    s, t, sibling = place(n, q)
    barrier = pltpu.get_barrier_semaphore()
    for i in range(1, n):
        pl.semaphore_signal(
            barrier, inc=1, device_id=(lax.rem(s + i, n), t), device_id_type=MESH
        )
    for d in range(1, q // 2):
        pl.semaphore_signal(
            barrier, inc=1, device_id=(s, lax.rem(t + 2 * d, q)), device_id_type=MESH
        )
    pl.semaphore_signal(barrier, inc=1, device_id=(s, sibling), device_id_type=MESH)
    return barrier, n - 1 + q // 2


def remote(src, dst, send_sem, recv_sem, device):
    return pltpu.make_async_remote_copy(
        src_ref=src,
        dst_ref=dst,
        send_sem=send_sem,
        recv_sem=recv_sem,
        device_id=device,
        device_id_type=MESH,
    )


def dispatch_kernel(
    n, q, ids_ref, w_ref, x_ref, g_ref, xo_ref, do_ref, p_ref,
    p01, send, buf, out_sem, s1, r1, sy, ry, ss, rs,
):
    s, t, sibling = place(n, q)
    ny = q // 2
    tok, cols = x_ref.shape
    total = send.shape[1]
    cap = total // n
    barrier, greeted = greet(n, q)

    ids0, ids1 = ids_ref[0:1, :], ids_ref[1:2, :]
    experts = lax.broadcasted_iota(jnp.int32, (n, tok), 0)
    named = jnp.logical_or(ids0 == experts, ids1 == experts)
    named_f = jnp.where(named, 1.0, 0.0)
    earlier = jnp.where(
        lax.broadcasted_iota(jnp.int32, (tok, tok), 0)
        < lax.broadcasted_iota(jnp.int32, (tok, tok), 1),
        1.0,
        0.0,
    )
    before = jnp.dot(
        named_f.astype(jnp.bfloat16),
        earlier.astype(jnp.bfloat16),
        preferred_element_type=jnp.float32,
    ).astype(jnp.int32)
    slots = lax.broadcasted_iota(jnp.int32, (cap, tok), 0)
    for e in range(n):
        here = before[e : e + 1, :] == slots
        c0 = jnp.where(jnp.logical_and(here, ids0 == e), 1.0, 0.0)
        c1 = jnp.where(jnp.logical_and(here, ids1 == e), 1.0, 0.0)
        rows = slice(e * cap, (e + 1) * cap)
        p01[rows, 0:tok] = c0.astype(jnp.bfloat16)
        p01[rows, tok : 2 * tok] = c1.astype(jnp.bfloat16)
        p_ref[rows, :] = (c0 + c1).astype(jnp.bfloat16)
    grad = g_ref[...].astype(jnp.float32)
    weighted = jnp.concatenate(
        [
            (w_ref[:, 0:1] * grad).astype(jnp.bfloat16),
            (w_ref[:, 1:2] * grad).astype(jnp.bfloat16),
        ],
        axis=0,
    )
    send[0] = jnp.dot(p_ref[...], x_ref[...], preferred_element_type=jnp.float32).astype(
        jnp.bfloat16
    )
    send[1] = jnp.dot(p01[...], weighted, preferred_element_type=jnp.float32).astype(jnp.bfloat16)

    def at_rows(j):
        return pl.ds(pl.multiple_of(j * cap, cap), cap)

    def block(j, tt):
        return buf.at[:, at_rows(j), pl.ds(pl.multiple_of(tt * cols, cols), cols)]

    def first(i):
        e = lax.rem(s + i, n)
        return remote(send.at[:, at_rows(e)], block(s, t), s1.at[i], r1.at[i], (e, t))

    def across(i, d):
        j = lax.rem(s - i + n, n)
        b = block(j, t)
        return remote(b, b, sy.at[i, d - 1], ry.at[i, d - 1], (s, lax.rem(t + 2 * d, q)))

    def beside(i, d):
        j = lax.rem(s - i + n, n)
        b = block(j, lax.rem(t - 2 * d + q, q))
        return remote(b, b, ss.at[i, d], rs.at[i, d], (s, sibling))

    pl.semaphore_wait(barrier, greeted)
    own = pltpu.make_async_copy(send.at[:, at_rows(s)], block(s, t), s1.at[0])
    own.start()
    for i in range(1, n):
        first(i).start()

    def forward(i):
        for d in range(1, ny):
            across(i, d).wait_recv()
            beside(i, d).start()

    outs = []

    def drain(i):
        j = lax.rem(s - i + n, n)
        for d in range(ny):
            beside(i, d).wait_recv()
        for a, ref in enumerate((xo_ref, do_ref)):
            copy = pltpu.make_async_copy(
                buf.at[a, at_rows(j)], ref.at[at_rows(j)], out_sem.at[i, a]
            )
            copy.start()
            outs.append(copy)

    for i in range(n):
        if i == 0:
            own.wait()
        else:
            first(i).wait_recv()
        for d in range(1, ny):
            across(i, d).start()
        beside(i, 0).start()
        if i >= 1:
            forward(i - 1)
        if i >= 2:
            drain(i - 2)
    forward(n - 1)
    for i in range(max(n - 2, 0), n):
        drain(i)
    for i in range(n):
        if i:
            first(i).wait_send()
        for d in range(1, ny):
            across(i, d).wait_send()
        for d in range(ny):
            beside(i, d).wait_send()
    for copy in outs:
        copy.wait()


def dispatch(n, q, ids_t, weight, x, g):
    tok, cols = x.shape
    total = 4 * tok
    ny = q // 2
    vmem = pl.BlockSpec(memory_space=pltpu.VMEM)
    hbm = pl.BlockSpec(memory_space=pl.ANY)
    dma = pltpu.SemaphoreType.DMA
    rows = jax.ShapeDtypeStruct((total, q * cols), jnp.bfloat16)
    return pl.pallas_call(
        functools.partial(dispatch_kernel, n, q),
        out_shape=(rows, rows, jax.ShapeDtypeStruct((total, tok), jnp.bfloat16)),
        in_specs=[vmem] * 4,
        out_specs=(hbm, hbm, vmem),
        scratch_shapes=[
            pltpu.VMEM((total, 2 * tok), jnp.bfloat16),
            pltpu.VMEM((2, total, cols), jnp.bfloat16),
            pltpu.VMEM((2, total, q * cols), jnp.bfloat16),
            dma((n, 2)),
            dma((n,)),
            dma((n,)),
            dma((n, max(ny - 1, 1))),
            dma((n, max(ny - 1, 1))),
            dma((n, ny)),
            dma((n, ny)),
        ],
        compiler_params=pltpu.CompilerParams(collective_id=0, has_side_effects=True),
        name="dispatch",
    )(ids_t, weight, x, g)


def combine_kernel(
    n, q, part_ref, p_ref, g_ref, b_ref, co_ref, c_ref, v_ref, taps_ref, w_hbm,
    gout_ref, gb_ref, gc_ref, gv_ref,
    rsib, pair, ryb, fin, ret, full_h, h_t, all_t, all_m, w_ref, edge, got, padded, w_sem,
    ss, rs, sy, ry, s3, r3, sm, rm, sp, rp, shy, rhy, shs, rhs, sa, ra, se, re,
):
    s, t, sibling = place(n, q)
    partner = s + 1 - 2 * lax.rem(s, 2)
    ny = q // 2
    tok, cols = g_ref.shape
    total, width = part_ref.shape
    cap = total // n
    share = width // n
    barrier, greeted = greet(n, q)
    w_copy = pltpu.make_async_copy(w_hbm, w_ref, w_sem)
    w_copy.start()
    all_m[s] = (b_ref[...].astype(jnp.float32) * co_ref[...].astype(jnp.float32)).astype(
        jnp.bfloat16
    )

    def at_rows(j):
        return pl.ds(pl.multiple_of(j * cap, cap), cap)

    def at_cols(tt):
        return pl.ds(pl.multiple_of(tt * cols, cols), cols)

    def beside(i, d):
        j = lax.rem(s + i, n)
        theirs = lax.rem(sibling + 2 * d, q)
        return remote(
            part_ref.at[at_rows(j), at_cols(theirs)],
            rsib.at[d, at_rows(j)],
            ss.at[i, d],
            rs.at[i, d],
            (s, sibling),
        )

    def across(i, d):
        j = lax.rem(s + i, n)
        return remote(
            pair.at[d - 1, at_rows(j)],
            ryb.at[d - 1, at_rows(j)],
            sy.at[i, d - 1],
            ry.at[i, d - 1],
            (s, lax.rem(t + 2 * d, q)),
        )

    def back(i):
        j = lax.rem(s + i, n)
        return remote(fin.at[at_rows(j)], ret.at[at_rows(s)], s3.at[i], r3.at[i], (j, t))

    def mixed_far(i):
        return remote(
            all_m.at[s], all_m.at[s], sm.at[i // 2], rm.at[i // 2], (lax.rem(s + i, n), t)
        )

    def mixed_near(i):
        b = all_m.at[lax.rem(s - i + n, n)]
        return remote(b, b, sp.at[i // 2], rp.at[i // 2], (partner, t))

    def h_across(d):
        b = full_h.at[:, at_cols(t)]
        return remote(b, b, shy.at[d - 1], rhy.at[d - 1], (s, lax.rem(t + 2 * d, q)))

    def h_beside(d):
        b = full_h.at[:, at_cols(lax.rem(t - 2 * d + q, q))]
        return remote(b, b, shs.at[d], rhs.at[d], (s, sibling))

    def h_share(j):
        return pl.ds(pl.multiple_of(j * share, share), share)

    def h_far(i):
        j = lax.rem(s + i, n)
        return remote(h_t.at[h_share(j)], all_t.at[s], sa.at[i], ra.at[i], (j, t))

    def halo(k):
        there = lax.rem(s + 1, n) if k == 0 else lax.rem(s - 1 + n, n)
        return remote(edge.at[k], got.at[k], se.at[k], re.at[k], (there, t))

    def mine(j, d):
        value = part_ref[at_rows(j), at_cols(lax.rem(t + 2 * d, q))].astype(jnp.float32)
        return value + rsib[d, at_rows(j), :].astype(jnp.float32)

    order = [i % n for i in range(1, n + 1)]
    pl.semaphore_wait(barrier, greeted)
    for i in order:
        for d in [*range(1, ny), 0]:
            beside(i, d).start()
    for i in range(2, n, 2):
        mixed_far(i).start()
    mixed_near(0).start()

    def finish(i):
        j = lax.rem(s + i, n)
        beside(i, 0).wait_recv()
        value = mine(j, 0)
        for d in range(1, ny):
            across(i, d).wait_recv()
            value = value + ryb[d - 1, at_rows(j), :].astype(jnp.float32)
        value = value.astype(jnp.bfloat16)
        if i == 0:
            ret[at_rows(s), :] = value
        else:
            fin[at_rows(j), :] = value
            back(i).start()

    for k, i in enumerate(order):
        j = lax.rem(s + i, n)
        for d in range(1, ny):
            beside(i, d).wait_recv()
            pair[d - 1, at_rows(j), :] = mine(j, d).astype(jnp.bfloat16)
            across(i, d).start()
        if k >= 1:
            finish(order[k - 1])
    finish(order[-1])
    for i in range(2, n, 2):
        mixed_far(i).wait_recv()
        mixed_near(i).start()
    for i in range(1, n):
        back(i).wait_recv()
    moe = lax.dot_general(
        p_ref[...], ret[...], (((0,), (0,)), ((), ())), preferred_element_type=jnp.float32
    )
    full_h[:, at_cols(t)] = (g_ref[...].astype(jnp.float32) + moe).astype(jnp.bfloat16)
    for d in range(1, ny):
        h_across(d).start()
    h_beside(0).start()
    w_copy.wait()
    for d in range(1, ny):
        h_across(d).wait_recv()
        h_beside(d).start()
    for d in range(ny):
        h_beside(d).wait_recv()
    for k in range(q):
        here = slice(k * cols, (k + 1) * cols)
        h_t[here, :] = full_h[:, here].astype(jnp.float32).T.astype(jnp.bfloat16)
    for i in range(1, n):
        h_far(i).start()
    all_t[s] = h_t[h_share(s), :]
    grad_z = jnp.dot(full_h[...], w_ref[...], preferred_element_type=jnp.float32)
    dconv = (grad_z * b_ref[...].astype(jnp.float32)).astype(jnp.bfloat16).astype(jnp.float32)
    edge[0] = jnp.broadcast_to(dconv[tok - 1 : tok, :], (8, cols))
    edge[1] = jnp.broadcast_to(dconv[0:1, :], (8, cols))
    halo(0).start()
    halo(1).start()
    gb_ref[...] = (grad_z * co_ref[...].astype(jnp.float32)).astype(jnp.bfloat16)
    padded[8 : 8 + tok, :] = dconv
    halo(0).wait_recv()
    halo(1).wait_recv()
    padded[0:8, :] = jnp.where(s > 0, got[0], 0.0)
    padded[8 + tok : 16 + tok, :] = jnp.where(s < n - 1, got[1], 0.0)
    grad_u = (
        taps_ref[0:1, :] * padded[9 : 9 + tok, :]
        + taps_ref[1:2, :] * padded[8 : 8 + tok, :]
        + taps_ref[2:3, :] * padded[7 : 7 + tok, :]
    )
    gc_ref[...] = (grad_u * v_ref[...].astype(jnp.float32)).astype(jnp.bfloat16)
    gv_ref[...] = (grad_u * c_ref[...].astype(jnp.float32)).astype(jnp.bfloat16)
    for i in range(0, n, 2):
        mixed_near(i).wait_recv()
    for i in range(1, n):
        h_far(i).wait_recv()
    total_out = jnp.zeros((share, cols), jnp.float32)
    for k in range(n):
        total_out = total_out + jnp.dot(all_t[k], all_m[k], preferred_element_type=jnp.float32)
    gout_ref[...] = total_out
    for i in range(n):
        if i:
            back(i).wait_send()
            h_far(i).wait_send()
        if i % 2 == 0:
            mixed_near(i).wait_send()
            if i:
                mixed_far(i).wait_send()
        for d in range(1, ny):
            across(i, d).wait_send()
        for d in range(ny):
            beside(i, d).wait_send()
    for d in range(ny):
        if d:
            h_across(d).wait_send()
        h_beside(d).wait_send()
    halo(0).wait_send()
    halo(1).wait_send()


def combine(n, q, part, p, g, gate_b, conv_out, gate_c, value_v, taps, out_proj):
    total, width = part.shape
    tok, cols = g.shape
    share = width // n
    ny = q // 2
    far = max(ny - 1, 1)
    vmem = pl.BlockSpec(memory_space=pltpu.VMEM)
    dma = pltpu.SemaphoreType.DMA
    half = jnp.bfloat16
    like = jax.ShapeDtypeStruct(g.shape, half)
    sems = [(n, ny), (n, far), (n,), (n // 2,), (n // 2,), (far,), (ny,), (n,), (2,)]
    return pl.pallas_call(
        functools.partial(combine_kernel, n, q),
        out_shape=(jax.ShapeDtypeStruct((share, cols), jnp.float32), like, like, like),
        in_specs=[vmem] * 8 + [pl.BlockSpec(memory_space=pl.ANY)],
        out_specs=(vmem,) * 4,
        scratch_shapes=[
            pltpu.VMEM((ny, total, cols), half),
            pltpu.VMEM((far, total, cols), half),
            pltpu.VMEM((far, total, cols), half),
            pltpu.VMEM((total, cols), half),
            pltpu.VMEM((total, cols), half),
            pltpu.VMEM((tok, width), half),
            pltpu.VMEM((width, tok), half),
            pltpu.VMEM((n, share, tok), half),
            pltpu.VMEM((n, tok, cols), half),
            pltpu.VMEM(out_proj.shape, half),
            pltpu.VMEM((2, 8, cols), jnp.float32),
            pltpu.VMEM((2, 8, cols), jnp.float32),
            pltpu.VMEM((tok + 16, cols), jnp.float32),
            dma,
        ]
        + [dma(shape) for shape in sems for _ in range(2)],
        compiler_params=pltpu.CompilerParams(collective_id=1, has_side_effects=True),
        name="combine",
    )(part, p, g, gate_b, conv_out, gate_c, value_v, taps, out_proj)


def local(
    out_grad,
    moe_input,
    route_weight,
    route_ids,
    gate_proj,
    up_proj,
    down_proj,
    out_proj,
    conv_out,
    gate_b,
    gate_c,
    value_v,
    conv_taps,
):
    n = lax.axis_size("sp")
    q = lax.axis_size("tp")
    xin, dyin, slots = dispatch(n, q, route_ids.T, route_weight, moe_input, out_grad)
    w_gate = gate_proj[0]
    w_up = up_proj[0]
    w_down = down_proj[0]
    gate = jnp.dot(xin, w_gate, preferred_element_type=jnp.float32)
    upval = jnp.dot(xin, w_up, preferred_element_type=jnp.float32)
    sig = jax.nn.sigmoid(gate)
    act = gate * sig
    hidden = (act * upval).astype(jnp.bfloat16)
    dhid = jnp.dot(dyin, w_down.T, preferred_element_type=jnp.float32)
    dgate = (dhid * upval * (sig * (1.0 + gate * (1.0 - sig)))).astype(jnp.bfloat16)
    dup = (dhid * act).astype(jnp.bfloat16)
    partial_value = jnp.dot(dgate, w_gate.T, preferred_element_type=jnp.float32) + jnp.dot(
        dup, w_up.T, preferred_element_type=jnp.float32
    )
    grad_out, grad_b, grad_c, grad_v = combine(
        n,
        q,
        partial_value.astype(jnp.bfloat16),
        slots,
        out_grad,
        gate_b,
        conv_out,
        gate_c,
        value_v,
        conv_taps,
        out_proj,
    )
    grad_down = jnp.dot(hidden.T, dyin, preferred_element_type=jnp.float32).astype(jnp.bfloat16)
    grad_gate = jnp.dot(xin.T, dgate, preferred_element_type=jnp.float32).astype(jnp.bfloat16)
    grad_up = jnp.dot(xin.T, dup, preferred_element_type=jnp.float32).astype(jnp.bfloat16)
    return (grad_gate[None], grad_up[None], grad_down[None], grad_out, grad_b, grad_c, grad_v)


def solution(mesh):
    in_specs = (
        P("sp", "tp"),
        P("sp", "tp"),
        P("sp", None),
        P("sp", None),
        P("sp", None, "tp"),
        P("sp", None, "tp"),
        P("sp", "tp", None),
        P(None, "tp"),
        P("sp", "tp"),
        P("sp", "tp"),
        P("sp", "tp"),
        P("sp", "tp"),
        P(None, "tp"),
    )
    out_specs = (
        P("sp", None, "tp"),
        P("sp", None, "tp"),
        P("sp", "tp", None),
        P("sp", "tp"),
        P("sp", "tp"),
        P("sp", "tp"),
        P("sp", "tp"),
    )
    return jax.shard_map(local, mesh=mesh, in_specs=in_specs, out_specs=out_specs, check_vma=False)
```

```python
import functools

import jax
import jax.numpy as jnp
from jax import lax
from jax.experimental import pallas as pl
from jax.experimental.pallas import tpu as pltpu
from jax.sharding import PartitionSpec as P

MESH = pl.DeviceIdType.MESH


def place(n, q):
    s, t = lax.axis_index("sp"), lax.axis_index("tp")
    sibling = t + 1 - 2 * lax.rem(t, 2)
    return s, t, sibling


def greet(n, q):
    s, t, sibling = place(n, q)
    barrier = pltpu.get_barrier_semaphore()
    for i in range(1, n):
        pl.semaphore_signal(
            barrier, inc=1, device_id=(lax.rem(s + i, n), t), device_id_type=MESH
        )
    for d in range(1, q // 2):
        pl.semaphore_signal(
            barrier, inc=1, device_id=(s, lax.rem(t + 2 * d, q)), device_id_type=MESH
        )
    pl.semaphore_signal(barrier, inc=1, device_id=(s, sibling), device_id_type=MESH)
    return barrier, n - 1 + q // 2


def remote(src, dst, send_sem, recv_sem, device):
    return pltpu.make_async_remote_copy(
        src_ref=src,
        dst_ref=dst,
        send_sem=send_sem,
        recv_sem=recv_sem,
        device_id=device,
        device_id_type=MESH,
    )


def dispatch_kernel(
    n, q, ids_ref, w_ref, x_ref, g_ref, xo_ref, do_ref, p_ref,
    p01, send, buf, out_sem, s1, r1, sy, ry, ss, rs,
):
    s, t, sibling = place(n, q)
    ny = q // 2
    tok, cols = x_ref.shape
    total = send.shape[1]
    cap = total // n
    barrier, greeted = greet(n, q)

    ids0, ids1 = ids_ref[0:1, :], ids_ref[1:2, :]
    experts = lax.broadcasted_iota(jnp.int32, (n, tok), 0)
    named = jnp.logical_or(ids0 == experts, ids1 == experts)
    named_f = jnp.where(named, 1.0, 0.0)
    earlier = jnp.where(
        lax.broadcasted_iota(jnp.int32, (tok, tok), 0)
        < lax.broadcasted_iota(jnp.int32, (tok, tok), 1),
        1.0,
        0.0,
    )
    before = jnp.dot(
        named_f.astype(jnp.bfloat16),
        earlier.astype(jnp.bfloat16),
        preferred_element_type=jnp.float32,
    ).astype(jnp.int32)
    slots = lax.broadcasted_iota(jnp.int32, (cap, tok), 0)
    for e in range(n):
        here = before[e : e + 1, :] == slots
        c0 = jnp.where(jnp.logical_and(here, ids0 == e), 1.0, 0.0)
        c1 = jnp.where(jnp.logical_and(here, ids1 == e), 1.0, 0.0)
        rows = slice(e * cap, (e + 1) * cap)
        p01[rows, 0:tok] = c0.astype(jnp.bfloat16)
        p01[rows, tok : 2 * tok] = c1.astype(jnp.bfloat16)
        p_ref[rows, :] = (c0 + c1).astype(jnp.bfloat16)
    grad = g_ref[...].astype(jnp.float32)
    weighted = jnp.concatenate(
        [
            (w_ref[:, 0:1] * grad).astype(jnp.bfloat16),
            (w_ref[:, 1:2] * grad).astype(jnp.bfloat16),
        ],
        axis=0,
    )
    send[0] = jnp.dot(p_ref[...], x_ref[...], preferred_element_type=jnp.float32).astype(
        jnp.bfloat16
    )
    send[1] = jnp.dot(p01[...], weighted, preferred_element_type=jnp.float32).astype(jnp.bfloat16)

    def at_rows(j):
        return pl.ds(pl.multiple_of(j * cap, cap), cap)

    def block(j, tt):
        return buf.at[:, at_rows(j), pl.ds(pl.multiple_of(tt * cols, cols), cols)]

    def first(i):
        e = lax.rem(s + i, n)
        return remote(send.at[:, at_rows(e)], block(s, t), s1.at[i], r1.at[i], (e, t))

    def across(i, d):
        j = lax.rem(s - i + n, n)
        b = block(j, t)
        return remote(b, b, sy.at[i, d - 1], ry.at[i, d - 1], (s, lax.rem(t + 2 * d, q)))

    def beside(i, d):
        j = lax.rem(s - i + n, n)
        b = block(j, lax.rem(t - 2 * d + q, q))
        return remote(b, b, ss.at[i, d], rs.at[i, d], (s, sibling))

    pl.semaphore_wait(barrier, greeted)
    own = pltpu.make_async_copy(send.at[:, at_rows(s)], block(s, t), s1.at[0])
    own.start()
    for i in range(1, n):
        first(i).start()

    def forward(i):
        for d in range(1, ny):
            across(i, d).wait_recv()
            beside(i, d).start()

    outs = []

    def drain(i):
        j = lax.rem(s - i + n, n)
        for d in range(ny):
            beside(i, d).wait_recv()
        for a, ref in enumerate((xo_ref, do_ref)):
            copy = pltpu.make_async_copy(
                buf.at[a, at_rows(j)], ref.at[at_rows(j)], out_sem.at[i, a]
            )
            copy.start()
            outs.append(copy)

    for i in range(n):
        if i == 0:
            own.wait()
        else:
            first(i).wait_recv()
        for d in range(1, ny):
            across(i, d).start()
        beside(i, 0).start()
        if i >= 1:
            forward(i - 1)
        if i >= 2:
            drain(i - 2)
    forward(n - 1)
    for i in range(max(n - 2, 0), n):
        drain(i)
    for i in range(n):
        if i:
            first(i).wait_send()
        for d in range(1, ny):
            across(i, d).wait_send()
        for d in range(ny):
            beside(i, d).wait_send()
    for copy in outs:
        copy.wait()


def dispatch(n, q, ids_t, weight, x, g):
    tok, cols = x.shape
    total = 4 * tok
    ny = q // 2
    vmem = pl.BlockSpec(memory_space=pltpu.VMEM)
    hbm = pl.BlockSpec(memory_space=pl.ANY)
    dma = pltpu.SemaphoreType.DMA
    rows = jax.ShapeDtypeStruct((total, q * cols), jnp.bfloat16)
    return pl.pallas_call(
        functools.partial(dispatch_kernel, n, q),
        out_shape=(rows, rows, jax.ShapeDtypeStruct((total, tok), jnp.bfloat16)),
        in_specs=[vmem] * 4,
        out_specs=(hbm, hbm, vmem),
        scratch_shapes=[
            pltpu.VMEM((total, 2 * tok), jnp.bfloat16),
            pltpu.VMEM((2, total, cols), jnp.bfloat16),
            pltpu.VMEM((2, total, q * cols), jnp.bfloat16),
            dma((n, 2)),
            dma((n,)),
            dma((n,)),
            dma((n, max(ny - 1, 1))),
            dma((n, max(ny - 1, 1))),
            dma((n, ny)),
            dma((n, ny)),
        ],
        compiler_params=pltpu.CompilerParams(collective_id=0, has_side_effects=True),
        name="dispatch",
    )(ids_t, weight, x, g)


def combine_kernel(
    n, q, part_ref, p_ref, g_ref, b_ref, co_ref, c_ref, v_ref, taps_ref, w_hbm,
    x_hbm, dy_hbm, hid_hbm, dg_hbm, du_hbm,
    gout_ref, gb_ref, gc_ref, gv_ref, ggate_hbm, gup_hbm, gdown_hbm,
    rsib, pair, ryb, fin, ret, full_h, h_t, all_t, all_m, w_ref, edge, got, padded,
    x_v, dy_v, hid_v, dg_v, du_v, ggate_v, gup_v, gdown_v, in_sem, o_sem, w_sem,
    ss, rs, sy, ry, s3, r3, sm, rm, sp, rp, shy, rhy, shs, rhs, sa, ra, se, re,
):
    s, t, sibling = place(n, q)
    partner = s + 1 - 2 * lax.rem(s, 2)
    ny = q // 2
    tok, cols = g_ref.shape
    total, width = part_ref.shape
    cap = total // n
    share = width // n
    barrier, greeted = greet(n, q)
    w_copy = pltpu.make_async_copy(w_hbm, w_ref, w_sem)
    loads = [
        pltpu.make_async_copy(source, target, in_sem.at[k])
        for k, (source, target) in enumerate(
            zip((hid_hbm, dy_hbm, x_hbm, dg_hbm, du_hbm), (hid_v, dy_v, x_v, dg_v, du_v))
        )
    ]
    w_copy.start()
    for load in loads:
        load.start()
    all_m[s] = (b_ref[...].astype(jnp.float32) * co_ref[...].astype(jnp.float32)).astype(
        jnp.bfloat16
    )

    def at_rows(j):
        return pl.ds(pl.multiple_of(j * cap, cap), cap)

    def at_cols(tt):
        return pl.ds(pl.multiple_of(tt * cols, cols), cols)

    def beside(i, d):
        j = lax.rem(s + i, n)
        theirs = lax.rem(sibling + 2 * d, q)
        return remote(
            part_ref.at[at_rows(j), at_cols(theirs)],
            rsib.at[d, at_rows(j)],
            ss.at[i, d],
            rs.at[i, d],
            (s, sibling),
        )

    def across(i, d):
        j = lax.rem(s + i, n)
        return remote(
            pair.at[d - 1, at_rows(j)],
            ryb.at[d - 1, at_rows(j)],
            sy.at[i, d - 1],
            ry.at[i, d - 1],
            (s, lax.rem(t + 2 * d, q)),
        )

    def back(i):
        j = lax.rem(s + i, n)
        return remote(fin.at[at_rows(j)], ret.at[at_rows(s)], s3.at[i], r3.at[i], (j, t))

    def mixed_far(i):
        return remote(
            all_m.at[s], all_m.at[s], sm.at[i // 2], rm.at[i // 2], (lax.rem(s + i, n), t)
        )

    def mixed_near(i):
        b = all_m.at[lax.rem(s - i + n, n)]
        return remote(b, b, sp.at[i // 2], rp.at[i // 2], (partner, t))

    def h_across(d):
        b = full_h.at[:, at_cols(t)]
        return remote(b, b, shy.at[d - 1], rhy.at[d - 1], (s, lax.rem(t + 2 * d, q)))

    def h_beside(d):
        b = full_h.at[:, at_cols(lax.rem(t - 2 * d + q, q))]
        return remote(b, b, shs.at[d], rhs.at[d], (s, sibling))

    def h_share(j):
        return pl.ds(pl.multiple_of(j * share, share), share)

    def h_far(i):
        j = lax.rem(s + i, n)
        return remote(h_t.at[h_share(j)], all_t.at[s], sa.at[i], ra.at[i], (j, t))

    def halo(k):
        there = lax.rem(s + 1, n) if k == 0 else lax.rem(s - 1 + n, n)
        return remote(edge.at[k], got.at[k], se.at[k], re.at[k], (there, t))

    over_rows = (((0,), (0,)), ((), ()))
    stores = [
        pltpu.make_async_copy(source, target, o_sem.at[k])
        for k, (source, target) in enumerate(
            zip((gdown_v, ggate_v, gup_v), (gdown_hbm, ggate_hbm, gup_hbm))
        )
    ]

    def grad_step(left, right, target):
        def step(k, _):
            here = at_cols(k)
            target[:, here] = lax.dot_general(
                left[...], right[:, here], over_rows, preferred_element_type=jnp.float32
            ).astype(jnp.bfloat16)
            return 0

        return step

    def mine(j, d):
        value = part_ref[at_rows(j), at_cols(lax.rem(t + 2 * d, q))].astype(jnp.float32)
        return value + rsib[d, at_rows(j), :].astype(jnp.float32)

    order = [i % n for i in range(1, n + 1)]
    pl.semaphore_wait(barrier, greeted)
    for i in order:
        for d in [*range(1, ny), 0]:
            beside(i, d).start()
    for i in range(2, n, 2):
        mixed_far(i).start()
    mixed_near(0).start()

    def finish(i):
        j = lax.rem(s + i, n)
        beside(i, 0).wait_recv()
        value = mine(j, 0)
        for d in range(1, ny):
            across(i, d).wait_recv()
            value = value + ryb[d - 1, at_rows(j), :].astype(jnp.float32)
        value = value.astype(jnp.bfloat16)
        if i == 0:
            ret[at_rows(s), :] = value
        else:
            fin[at_rows(j), :] = value
            back(i).start()

    for k, i in enumerate(order):
        j = lax.rem(s + i, n)
        for d in range(1, ny):
            beside(i, d).wait_recv()
            pair[d - 1, at_rows(j), :] = mine(j, d).astype(jnp.bfloat16)
            across(i, d).start()
        if k >= 1:
            finish(order[k - 1])
    finish(order[-1])
    for i in range(2, n, 2):
        mixed_far(i).wait_recv()
        mixed_near(i).start()
    for load in loads:
        load.wait()
    lax.fori_loop(0, q, grad_step(hid_v, dy_v, gdown_v), 0)
    stores[0].start()
    for i in range(1, n):
        back(i).wait_recv()
    moe = lax.dot_general(
        p_ref[...], ret[...], (((0,), (0,)), ((), ())), preferred_element_type=jnp.float32
    )
    full_h[:, at_cols(t)] = (g_ref[...].astype(jnp.float32) + moe).astype(jnp.bfloat16)
    for d in range(1, ny):
        h_across(d).start()
    h_beside(0).start()
    w_copy.wait()
    for d in range(1, ny):
        h_across(d).wait_recv()
        h_beside(d).start()
    for d in range(ny):
        h_beside(d).wait_recv()
    for k in range(q):
        here = slice(k * cols, (k + 1) * cols)
        h_t[here, :] = full_h[:, here].astype(jnp.float32).T.astype(jnp.bfloat16)
    for i in range(1, n):
        h_far(i).start()
    all_t[s] = h_t[h_share(s), :]
    grad_z = jnp.dot(full_h[...], w_ref[...], preferred_element_type=jnp.float32)
    dconv = (grad_z * b_ref[...].astype(jnp.float32)).astype(jnp.bfloat16).astype(jnp.float32)
    edge[0] = jnp.broadcast_to(dconv[tok - 1 : tok, :], (8, cols))
    edge[1] = jnp.broadcast_to(dconv[0:1, :], (8, cols))
    halo(0).start()
    halo(1).start()
    gb_ref[...] = (grad_z * co_ref[...].astype(jnp.float32)).astype(jnp.bfloat16)
    padded[8 : 8 + tok, :] = dconv
    halo(0).wait_recv()
    halo(1).wait_recv()
    padded[0:8, :] = jnp.where(s > 0, got[0], 0.0)
    padded[8 + tok : 16 + tok, :] = jnp.where(s < n - 1, got[1], 0.0)
    grad_u = (
        taps_ref[0:1, :] * padded[9 : 9 + tok, :]
        + taps_ref[1:2, :] * padded[8 : 8 + tok, :]
        + taps_ref[2:3, :] * padded[7 : 7 + tok, :]
    )
    gc_ref[...] = (grad_u * v_ref[...].astype(jnp.float32)).astype(jnp.bfloat16)
    gv_ref[...] = (grad_u * c_ref[...].astype(jnp.float32)).astype(jnp.bfloat16)
    lax.fori_loop(0, q, grad_step(dg_v, x_v, ggate_v), 0)
    stores[1].start()
    lax.fori_loop(0, q, grad_step(du_v, x_v, gup_v), 0)
    stores[2].start()
    for i in range(0, n, 2):
        mixed_near(i).wait_recv()
    for i in range(1, n):
        h_far(i).wait_recv()
    total_out = jnp.zeros((share, cols), jnp.float32)
    for k in range(n):
        total_out = total_out + jnp.dot(all_t[k], all_m[k], preferred_element_type=jnp.float32)
    gout_ref[...] = total_out
    for i in range(n):
        if i:
            back(i).wait_send()
            h_far(i).wait_send()
        if i % 2 == 0:
            mixed_near(i).wait_send()
            if i:
                mixed_far(i).wait_send()
        for d in range(1, ny):
            across(i, d).wait_send()
        for d in range(ny):
            beside(i, d).wait_send()
    for d in range(ny):
        if d:
            h_across(d).wait_send()
        h_beside(d).wait_send()
    halo(0).wait_send()
    halo(1).wait_send()
    for store in stores:
        store.wait()


def combine(
    n, q, part, p, g, gate_b, conv_out, gate_c, value_v, taps, out_proj, x, dy, hid, dg, du
):
    total, width = part.shape
    tok, cols = g.shape
    share = width // n
    ny = q // 2
    far = max(ny - 1, 1)
    vmem = pl.BlockSpec(memory_space=pltpu.VMEM)
    dma = pltpu.SemaphoreType.DMA
    half = jnp.bfloat16
    like = jax.ShapeDtypeStruct(g.shape, half)
    hbm = pl.BlockSpec(memory_space=pl.ANY)
    units = hid.shape[1]
    tall = (units, width)
    sems = [(n, ny), (n, far), (n,), (n // 2,), (n // 2,), (far,), (ny,), (n,), (2,)]
    return pl.pallas_call(
        functools.partial(combine_kernel, n, q),
        out_shape=(
            jax.ShapeDtypeStruct((share, cols), jnp.float32),
            like,
            like,
            like,
            jax.ShapeDtypeStruct(tall, half),
            jax.ShapeDtypeStruct(tall, half),
            jax.ShapeDtypeStruct(tall, half),
        ),
        in_specs=[vmem] * 8 + [hbm] * 6,
        out_specs=(vmem,) * 4 + (hbm,) * 3,
        scratch_shapes=[
            pltpu.VMEM((ny, total, cols), half),
            pltpu.VMEM((far, total, cols), half),
            pltpu.VMEM((far, total, cols), half),
            pltpu.VMEM((total, cols), half),
            pltpu.VMEM((total, cols), half),
            pltpu.VMEM((tok, width), half),
            pltpu.VMEM((width, tok), half),
            pltpu.VMEM((n, share, tok), half),
            pltpu.VMEM((n, tok, cols), half),
            pltpu.VMEM(out_proj.shape, half),
            pltpu.VMEM((2, 8, cols), jnp.float32),
            pltpu.VMEM((2, 8, cols), jnp.float32),
            pltpu.VMEM((tok + 16, cols), jnp.float32),
            pltpu.VMEM((total, width), half),
            pltpu.VMEM((total, width), half),
            pltpu.VMEM((total, units), half),
            pltpu.VMEM((total, units), half),
            pltpu.VMEM((total, units), half),
            pltpu.VMEM(tall, half),
            pltpu.VMEM(tall, half),
            pltpu.VMEM(tall, half),
            dma((5,)),
            dma((3,)),
            dma,
        ]
        + [dma(shape) for shape in sems for _ in range(2)],
        compiler_params=pltpu.CompilerParams(collective_id=1, has_side_effects=True, vmem_limit_bytes=30 * 2**20),
        name="combine",
    )(part, p, g, gate_b, conv_out, gate_c, value_v, taps, out_proj, x, dy, hid, dg, du)


def local(
    out_grad,
    moe_input,
    route_weight,
    route_ids,
    gate_proj,
    up_proj,
    down_proj,
    out_proj,
    conv_out,
    gate_b,
    gate_c,
    value_v,
    conv_taps,
):
    n = lax.axis_size("sp")
    q = lax.axis_size("tp")
    xin, dyin, slots = dispatch(n, q, route_ids.T, route_weight, moe_input, out_grad)
    w_gate = gate_proj[0]
    w_up = up_proj[0]
    w_down = down_proj[0]
    gate = jnp.dot(xin, w_gate, preferred_element_type=jnp.float32)
    upval = jnp.dot(xin, w_up, preferred_element_type=jnp.float32)
    sig = jax.nn.sigmoid(gate)
    act = gate * sig
    hidden = (act * upval).astype(jnp.bfloat16)
    dhid = jnp.dot(dyin, w_down.T, preferred_element_type=jnp.float32)
    dgate = (dhid * upval * (sig * (1.0 + gate * (1.0 - sig)))).astype(jnp.bfloat16)
    dup = (dhid * act).astype(jnp.bfloat16)
    partial_value = jnp.dot(dgate, w_gate.T, preferred_element_type=jnp.float32) + jnp.dot(
        dup, w_up.T, preferred_element_type=jnp.float32
    )
    grad_out, grad_b, grad_c, grad_v, grad_gate, grad_up, grad_down = combine(
        n,
        q,
        partial_value.astype(jnp.bfloat16),
        slots,
        out_grad,
        gate_b,
        conv_out,
        gate_c,
        value_v,
        conv_taps,
        out_proj,
        xin,
        dyin,
        hidden,
        dgate,
        dup,
    )
    return (grad_gate.T[None], grad_up.T[None], grad_down[None], grad_out, grad_b, grad_c, grad_v)


def solution(mesh):
    in_specs = (
        P("sp", "tp"),
        P("sp", "tp"),
        P("sp", None),
        P("sp", None),
        P("sp", None, "tp"),
        P("sp", None, "tp"),
        P("sp", "tp", None),
        P(None, "tp"),
        P("sp", "tp"),
        P("sp", "tp"),
        P("sp", "tp"),
        P("sp", "tp"),
        P(None, "tp"),
    )
    out_specs = (
        P("sp", None, "tp"),
        P("sp", None, "tp"),
        P("sp", "tp", None),
        P("sp", "tp"),
        P("sp", "tp"),
        P("sp", "tp"),
        P("sp", "tp"),
    )
    return jax.shard_map(local, mesh=mesh, in_specs=in_specs, out_specs=out_specs, check_vma=False)
```
